32 devices in a mesh: grp: 2 (over y), ep: 16 (over z, x, core), tp: 1.
Axes of the slice: x: 2, y: 2, z: 4, core: 2. Of those that a mesh axis runs over, the one named last changes fastest.
Arguments:
- hidden: bfloat16 [256, 2048], P(('grp', 'ep'), 'tp'), parts along dimension 0, may hold values from -6 to 6
- head_input_projected: bfloat16 [256, 2048], P(('grp', 'ep'), 'tp'), parts along dimension 0, may hold values from -6 to 6
- output_gate_projected: bfloat16 [256, 2048], P(('grp', 'ep'), 'tp'), parts along dimension 0, may hold values from -6 to 6
- input_map_projected: bfloat16 [256, 256], P(('grp', 'ep'), 'tp'), parts along dimension 0, may hold values from -0.59765625 to 0.59765625
- output_map_projected: bfloat16 [256, 256], P(('grp', 'ep'), 'tp'), parts along dimension 0, may hold values from -6 to 6
- raw_step_size: bfloat16 [256, 32], P(('grp', 'ep'), 'tp'), parts along dimension 0, may hold values from -5 to 5
- convolution_history: bfloat16 [256, 3, 2048], P(('grp', 'ep'), None, 'tp'), parts along dimension 0, may hold values from -6 to 6
- convolution_kernel: bfloat16 [4, 2048], P(None, 'tp'), may hold values from -3 to 3
- recurrent_state_matrix: float32 [256, 32, 64, 64], P(('grp', 'ep'), 'tp'), parts along dimension 0, may hold values from -0.6 to 0.6
- head_decay_rate: float32 [32], P('tp'), may hold values from 0.05 to 4
- extra_log_decay: float32 [256, 32], P(('grp', 'ep'), 'tp'), parts along dimension 0, may hold values from -0.7 to 0
- head_skip_weight: float32 [32], P('tp'), may hold values from 0.1 to 1.9
- output_matrix: bfloat16 [2048, 2048], P('tp'), may hold values from -0.125 to 0.125
- expert_norm_scale: bfloat16 [2048], replicated, may hold values from 0.099609375 to 1.8984375
- token_expert_index: int32 [256, 6], P(('grp', 'ep')), parts along dimension 0, may hold values from 0 to 15, all different within a row; in each aligned block of 8 rows (0 to 7, 8 to 15, ...) at most 6 rows name the same one
- token_expert_weight: float32 [256, 6], P(('grp', 'ep')), parts along dimension 0, may hold values from 0.2 to 1
- expert_gate_weight: bfloat16 [16, 2048, 704], P('ep', None, 'tp'), may hold values from -0.125 to 0.125
- expert_up_weight: bfloat16 [16, 2048, 704], P('ep', None, 'tp'), may hold values from -0.125 to 0.125
- expert_down_weight: bfloat16 [16, 704, 2048], P('ep', 'tp'), may hold values from -0.21875 to 0.21875
Outputs:
- layer_out: bfloat16 [256, 2048], P(('grp', 'ep'), 'tp'), parts along dimension 0
- new_state: float32 [256, 32, 64, 64], P(('grp', 'ep'), 'tp'), parts along dimension 0
- new_hist: bfloat16 [256, 3, 2048], P(('grp', 'ep'), None, 'tp'), parts along dimension 0
The draws below stay inside these ranges and needn't reach their ends.
There are 2 independent parts, one for each index of `grp`. The reference program is written for one: setup_inputs(seed, part) draws one part's arguments, and reference() takes and returns one part's arrays. A program takes and returns all parts, laid end to end along the dimension named above; an argument that names none is the same for every part. Nothing has to cross between parts.
Inputs may be any that keep to these rules, and one draw needn't show every extreme that they name: `token_expert_index`: in the rows of one device (8 rows), no expert is named more than 6 times, and one expert is named exactly 6 times in some blocks; a token names 6 different experts.
All inputs are finite; a program needn't handle non-finite values.
Results may differ from the reference program's by a relative error of at most 0.015.
Values may be sent and summed in bfloat16 or wider, within the bound.
A program may use at most 64 MiB of HBM per device.

```python
import math
import jax
import jax.numpy as jnp
import numpy as np
from jax import lax

D = 2048
MIXER_HEADS = 32
HEAD_DIM = 64
GROUPS = 4
STATE_DIM = 64
TAPS = 4
EXP_FF = 704
TOPK = 6
SEQ_DEV = 8
SEQUENCE_COUNT = 128
EXPERTS = 16
CAP = 6
INNER = 2048
N_TP = 1


def block_scale(rng, extent, split, least, largest):
    loudness, own = 1.0, jax.random.fold_in(rng, 6)
    for axis_at, shards_of in split:
        draws = jnp.exp(jax.random.uniform(jax.random.fold_in(own, axis_at), (shards_of,), jnp.float32, least / len(split), largest / len(split)))
        loudness = loudness * jnp.repeat(draws, extent[axis_at] // shards_of).reshape([-1 if axis == axis_at else 1 for axis in range(len(extent))])
    return loudness


def assign_block(key, own, number, rows, number_of, top, limit, skew):
    sequence = jax.random.permutation(key, number_of)
    heavy_load, ordinary = shares(number_of, rows * top, limit, skew, True), shares(number_of, rows * top, limit, skew, False)
    places = jnp.arange(number_of)

    def named(sizes, rotation):
        used = int((sizes > 0).sum())
        fixed = max(1, used // 4)
        moved = fixed + (places - fixed + rotation * (used - fixed)) % max(1, number_of - fixed)
        return jnp.zeros((number_of,), jnp.int32).at[sequence[jnp.where(places < fixed, places, moved)]].set(jnp.asarray(sizes, jnp.int32))

    sizes = jnp.where(number % 4 == 0, named(heavy_load, number // 4), named(ordinary, number - number // 4 - 1))
    mixed = jax.random.permutation(jax.random.fold_in(own, 3), number_of)
    giver, taker = mixed[0:number_of // 2 * 2:2], mixed[1:number_of // 2 * 2:2]
    slack = jnp.minimum(sizes[giver] - 1, limit - sizes[taker]) // 2
    slack = jnp.where((giver == sequence[0]) | (taker == sequence[0]) | (sizes[taker] == 0), 0, jnp.maximum(slack, 0))
    moved = jax.random.randint(jax.random.fold_in(own, 4), (number_of // 2,), 0, 1 << 20) % (slack + 1)
    sizes = sizes.at[giver].add(-moved).at[taker].add(moved)
    items = jnp.searchsorted(jnp.cumsum(sizes), jnp.arange(rows * top), side="right").astype(jnp.int32)
    grid = items.reshape(top, rows).T
    grid = grid[jax.random.permutation(jax.random.fold_in(own, 1), rows)]
    rotation = jax.random.randint(jax.random.fold_in(own, 2), (rows, 1), 0, top)
    return jnp.take_along_axis(grid, (jnp.arange(top)[None, :] + rotation) % top, axis=1)


def shares(amount, total, reach, slope, full):
    portions = [(1 << 20) // math.isqrt(grade ** slope) + 1 for grade in range(1, amount + 1)]
    largest = reach if full else min(reach, max(-(-total // amount), total * portions[0] // sum(portions)))
    least = 1 if total - largest >= amount - 1 else 0
    counts, spare = [largest] + [least] * (amount - 1), total - largest - least * (amount - 1)
    while spare > 0:
        movable = [i for i in range(1, amount) if counts[i] < largest] or [i for i in range(1, amount) if counts[i] < reach]
        whole, left = sum([portions[i] for i in movable]), spare
        for i in movable:
            addition = min(reach - counts[i], max(1, left * portions[i] // whole), spare)
            counts[i] = counts[i] + addition
            spare = spare - addition
    return np.array(counts)


def bell_draw(key, extent, spread, bound, split=(), dtype=jnp.bfloat16):
    gain = block_scale(key, extent, split, -0.22, 0.18) if split else 1.0
    values = jax.random.normal(key, extent, jnp.float32) * spread * gain
    return jnp.minimum(jnp.maximum(values, -bound), bound).astype(dtype)


def setup_inputs(seed: int = 0, part: int = 0) -> dict:
    streams_of = jax.random.split(jax.random.key(seed), 20)
    part_keys = jax.random.split(jax.random.fold_in(streams_of[19], part), 20)
    hidden = bell_draw(part_keys[0], (SEQUENCE_COUNT, D), 1.0, 6.0, ((0, 16),))
    head_input_projected = bell_draw(part_keys[1], (SEQUENCE_COUNT, INNER), 1.0, 6.0, ((0, 16),))
    output_gate_projected = bell_draw(part_keys[2], (SEQUENCE_COUNT, INNER), 1.0, 6.0, ((0, 16),))
    input_map_projected = bell_draw(part_keys[3], (SEQUENCE_COUNT, GROUPS * STATE_DIM), 0.1, 0.59765625, ((0, 16),))
    output_map_projected = bell_draw(part_keys[4], (SEQUENCE_COUNT, GROUPS * STATE_DIM), 1.0, 6.0, ((0, 16),))
    raw_step_size = bell_draw(part_keys[5], (SEQUENCE_COUNT, MIXER_HEADS), 1.0, 5.0, ((0, 16),))
    convolution_history = bell_draw(part_keys[6], (SEQUENCE_COUNT, TAPS - 1, INNER), 1.0, 6.0, ((0, 16),))
    convolution_kernel = bell_draw(streams_of[7], (TAPS, INNER), TAPS ** -0.5, 3.0)
    recurrent_state_matrix = bell_draw(part_keys[8], (SEQUENCE_COUNT, MIXER_HEADS, HEAD_DIM, STATE_DIM), 0.1, 0.6, ((0, 16),), jnp.float32)
    head_decay_rate = jnp.clip(jnp.exp(jax.random.uniform(streams_of[9], (MIXER_HEADS,), jnp.float32, math.log(0.05), math.log(4.0))), 0.05, 4.0)
    extra_log_decay = jnp.clip(-0.7 + 0.7 * jax.random.uniform(part_keys[10], (SEQUENCE_COUNT, MIXER_HEADS), jnp.float32) ** block_scale(part_keys[10], (SEQUENCE_COUNT, MIXER_HEADS), ((0, 16),), -0.2, 0.2), -0.7, 0.0)
    head_skip_weight = jnp.clip(1.0 + 0.18 * jax.random.normal(streams_of[11], (MIXER_HEADS,), jnp.float32), 0.1, 1.9)
    output_matrix = bell_draw(streams_of[12], (INNER, D), INNER ** -0.5, 0.125)
    expert_norm_scale = jnp.clip(1.0 + 0.18 * jax.random.normal(streams_of[13], (D,), jnp.float32), 0.099609375, 1.8984375).astype(jnp.bfloat16)
    token_expert_index_keys = jax.random.split(jax.random.fold_in(part_keys[14], 1), SEQUENCE_COUNT // SEQ_DEV)
    token_expert_index_turns = jax.random.permutation(jax.random.fold_in(part_keys[14], 3), SEQUENCE_COUNT // SEQ_DEV)
    token_expert_index = jax.vmap(lambda own, number: assign_block(jax.random.fold_in(part_keys[14], 2), own, number, SEQ_DEV, EXPERTS, TOPK, CAP, 2))(token_expert_index_keys, token_expert_index_turns).reshape((SEQUENCE_COUNT, TOPK))
    token_expert_weight = jnp.clip(0.2 + 0.8 * jax.random.uniform(part_keys[15], (SEQUENCE_COUNT, TOPK), jnp.float32) ** block_scale(part_keys[15], (SEQUENCE_COUNT, TOPK), ((0, 16),), -0.2, 0.2), 0.2, 1.0)
    expert_gate_weight = bell_draw(streams_of[16], (EXPERTS, D, EXP_FF), D ** -0.5, 0.125, ((0, 16),))
    expert_up_weight = bell_draw(streams_of[17], (EXPERTS, D, EXP_FF), D ** -0.5, 0.125, ((0, 16),))
    expert_down_weight = bell_draw(streams_of[18], (EXPERTS, EXP_FF, D), EXP_FF ** -0.5, 0.21875, ((0, 16),))
    return dict(hidden=hidden, head_input_projected=head_input_projected, output_gate_projected=output_gate_projected, input_map_projected=input_map_projected, output_map_projected=output_map_projected, raw_step_size=raw_step_size, convolution_history=convolution_history, convolution_kernel=convolution_kernel, recurrent_state_matrix=recurrent_state_matrix, head_decay_rate=head_decay_rate, extra_log_decay=extra_log_decay, head_skip_weight=head_skip_weight, output_matrix=output_matrix, expert_norm_scale=expert_norm_scale, token_expert_index=token_expert_index, token_expert_weight=token_expert_weight, expert_gate_weight=expert_gate_weight, expert_up_weight=expert_up_weight, expert_down_weight=expert_down_weight)


EPSILON = 1e-06

def reference(hidden, head_input_projected, output_gate_projected, input_map_projected, output_map_projected, raw_step_size, convolution_history, convolution_kernel, recurrent_state_matrix, head_decay_rate, extra_log_decay, head_skip_weight, output_matrix, expert_norm_scale, token_expert_index, token_expert_weight, expert_gate_weight, expert_up_weight, expert_down_weight):
    seq_total = hidden.shape[0]
    window = jnp.concatenate([convolution_history, head_input_projected[:, None, :]], axis=1)
    new_hist = window[:, 1:]
    conv = jax.nn.silu(lax.optimization_barrier(jnp.sum(window.astype(jnp.float32) * convolution_kernel.astype(jnp.float32)[None], axis=1)))
    discrete_update = jax.nn.softplus(raw_step_size.astype(jnp.float32))
    decay_factor = jnp.exp(-head_decay_rate[None, :] * discrete_update + extra_log_decay)
    per_group = MIXER_HEADS // GROUPS
    heads_in = conv.reshape(seq_total, MIXER_HEADS, HEAD_DIM)
    b_heads = jnp.repeat(input_map_projected.astype(jnp.float32).reshape(seq_total, GROUPS, STATE_DIM), per_group, axis=1)
    c_heads = jnp.repeat(output_map_projected.astype(jnp.float32).reshape(seq_total, GROUPS, STATE_DIM), per_group, axis=1)
    new_state = decay_factor[:, :, None, None] * recurrent_state_matrix + (discrete_update[:, :, None] * heads_in)[:, :, :, None] * b_heads[:, :, None, :]
    readout = jnp.einsum('shpn,shn->shp', new_state, c_heads) + head_skip_weight[None, :, None] * heads_in
    gated = (readout.reshape(seq_total, INNER) * jax.nn.silu(output_gate_projected.astype(jnp.float32))).astype(jnp.bfloat16)
    half_inner = INNER // N_TP
    mixed = jnp.zeros((seq_total, D), jnp.float32)
    for index in range(N_TP):
        part_mix = jnp.dot(gated[:, index * half_inner:(index + 1) * half_inner], output_matrix[index * half_inner:(index + 1) * half_inner], preferred_element_type=jnp.float32).astype(jnp.bfloat16)
        mixed = mixed + lax.optimization_barrier(part_mix).astype(jnp.float32)
    resid = (hidden.astype(jnp.float32) + mixed).astype(jnp.bfloat16)
    values = resid.astype(jnp.float32)
    inv_rms = lax.rsqrt(lax.optimization_barrier(jnp.mean(values * values, axis=-1, keepdims=True)) + EPSILON)
    normed = (values * expert_norm_scale.astype(jnp.float32)).astype(jnp.bfloat16)
    half_ff = EXP_FF // N_TP

    def one_token(inputs):
        row, scale, experts, weights = inputs
        total = jnp.zeros((D,), jnp.float32)
        for slot in range(TOPK):
            which = experts[slot]
            pre = scale * jnp.dot(row[None], expert_gate_weight[which], preferred_element_type=jnp.float32)
            lin = scale * jnp.dot(row[None], expert_up_weight[which], preferred_element_type=jnp.float32)
            act = (jax.nn.silu(pre) * lin).astype(jnp.bfloat16)
            down = expert_down_weight[which]
            summed = jnp.zeros((1, D), jnp.float32)
            for index in range(N_TP):
                part_out = jnp.dot(act[:, index * half_ff:(index + 1) * half_ff], down[index * half_ff:(index + 1) * half_ff], preferred_element_type=jnp.float32).astype(jnp.bfloat16)
                summed = summed + lax.optimization_barrier(part_out).astype(jnp.float32)
            result = summed.astype(jnp.bfloat16)
            total = total + weights[slot] * result[0].astype(jnp.float32)
        return total
    routed = lax.map(one_token, (normed, inv_rms[:, 0], token_expert_index, token_expert_weight))
    layer_out = (values + routed).astype(jnp.bfloat16)
    return (layer_out, new_state, new_hist)
```

```python
import functools

import jax
import jax.numpy as jnp
from jax import lax
from jax.experimental import pallas as pl
from jax.experimental.pallas import tpu as pltpu
from jax.sharding import PartitionSpec as P

STATE_DIM = 64
TOPK = 6


EPSILON = 1e-06


def slot_numbers(token_expert_index, capacity, experts):
    flat = token_expert_index.reshape(-1)
    onehot = (flat[:, None] == jnp.arange(experts, dtype=jnp.int32)[None, :]).astype(jnp.int32)
    before = jnp.cumsum(onehot, axis=0) - onehot
    ranks = jnp.sum(before * onehot, axis=1)
    return (flat * capacity + ranks).reshape(token_expert_index.shape)


def on_device(
    hidden,
    head_input_projected,
    output_gate_projected,
    input_map_projected,
    output_map_projected,
    raw_step_size,
    convolution_history,
    convolution_kernel,
    recurrent_state_matrix,
    head_decay_rate,
    extra_log_decay,
    head_skip_weight,
    output_matrix,
    expert_norm_scale,
    token_expert_index,
    token_expert_weight,
    expert_gate_weight,
    expert_up_weight,
    expert_down_weight,
):
    seq_count, inner_local = head_input_projected.shape
    heads_local = raw_step_size.shape[1]
    head_width = inner_local // heads_local
    groups_local = input_map_projected.shape[1] // STATE_DIM
    per_group = heads_local // groups_local
    half_width = hidden.shape[1]
    full_width = output_matrix.shape[1]
    ep_count = lax.axis_size("ep")
    window = jnp.concatenate([convolution_history, head_input_projected[:, None, :]], axis=1)
    new_hist = window[:, 1:]
    conv = jax.nn.silu(
        jnp.sum(window.astype(jnp.float32) * convolution_kernel.astype(jnp.float32)[None], axis=1)
    )
    positive_step_size = jax.nn.softplus(raw_step_size.astype(jnp.float32))
    decay_factor = jnp.exp(-head_decay_rate[None, :] * positive_step_size + extra_log_decay)
    heads_in = conv.reshape(seq_count, heads_local, head_width)
    b_heads = jnp.repeat(
        input_map_projected.astype(jnp.float32).reshape(seq_count, groups_local, STATE_DIM),
        per_group,
        axis=1,
    )
    c_heads = jnp.repeat(
        output_map_projected.astype(jnp.float32).reshape(seq_count, groups_local, STATE_DIM),
        per_group,
        axis=1,
    )
    new_state = (
        decay_factor[:, :, None, None] * recurrent_state_matrix
        + (positive_step_size[:, :, None] * heads_in)[:, :, :, None] * b_heads[:, :, None, :]
    )
    readout = (
        jnp.einsum("shpn,shn->shp", new_state, c_heads) + head_skip_weight[None, :, None] * heads_in
    )
    gated = (
        readout.reshape(seq_count, inner_local)
        * jax.nn.silu(output_gate_projected.astype(jnp.float32))
    ).astype(jnp.bfloat16)
    partial_value = jnp.dot(gated, output_matrix, preferred_element_type=jnp.float32)
    mixed = lax.psum_scatter(
        partial_value.astype(jnp.bfloat16), "tp", scatter_dimension=1, tiled=True
    ).astype(jnp.float32)
    resid = (hidden.astype(jnp.float32) + mixed).astype(jnp.bfloat16)
    capacity = min(seq_count, max(2, 2 * seq_count * TOPK // ep_count))
    total_slots = ep_count * capacity
    slot_ids = jnp.arange(total_slots, dtype=jnp.int32)
    slots = slot_numbers(token_expert_index, capacity, ep_count)
    hits = (slots[:, :, None] == slot_ids[None, None, :]).astype(jnp.float32)
    picks = jnp.sum(hits, axis=1).T.astype(jnp.bfloat16)
    whole_rows = lax.all_gather(resid, "tp", axis=1, tiled=True)
    outgoing = jnp.dot(picks, whole_rows, preferred_element_type=jnp.float32).astype(jnp.bfloat16)
    received = lax.all_to_all(
        outgoing.reshape(ep_count, capacity, full_width),
        "ep",
        split_axis=0,
        concat_axis=0,
        tiled=True,
    )
    expert_rows = received.reshape(total_slots, full_width)
    values = expert_rows.astype(jnp.float32)
    inv_rms = lax.rsqrt(jnp.mean(values * values, axis=1, keepdims=True) + EPSILON)
    scaled = (values * expert_norm_scale.astype(jnp.float32)[None, :]).astype(jnp.bfloat16)
    pre_gate = inv_rms * jnp.dot(scaled, expert_gate_weight[0], preferred_element_type=jnp.float32)
    pre_up = inv_rms * jnp.dot(scaled, expert_up_weight[0], preferred_element_type=jnp.float32)
    act = (jax.nn.silu(pre_gate) * pre_up).astype(jnp.bfloat16)
    down_part = jnp.dot(act, expert_down_weight[0], preferred_element_type=jnp.float32)
    expert_out = lax.psum_scatter(
        down_part.astype(jnp.bfloat16), "tp", scatter_dimension=1, tiled=True
    )
    back = lax.all_to_all(
        expert_out.reshape(ep_count, capacity, half_width),
        "ep",
        split_axis=0,
        concat_axis=0,
        tiled=True,
    )
    mixing = jnp.sum(hits * token_expert_weight[:, :, None], axis=1)
    routed = jnp.dot(
        mixing,
        back.reshape(total_slots, half_width).astype(jnp.float32),
        precision=lax.Precision.HIGHEST,
    )
    layer_out = (resid.astype(jnp.float32) + routed).astype(jnp.bfloat16)
    return (layer_out, new_state, new_hist)


F32, BF16 = jnp.float32, jnp.bfloat16
MESH = pl.DeviceIdType.MESH
LANES = 128
NT = (((1,), (1,)), ((), ()))
VMEM_SPEC = pl.BlockSpec(memory_space=pltpu.VMEM)
HBM_SPEC = pl.BlockSpec(memory_space=pltpu.HBM)
FIELD = LANES // 4
MIXER_VMEM = 40 * 1024 * 1024
EXPERT_VMEM = 40 * 1024 * 1024


def dot(a, b):
    return jnp.dot(a, b, preferred_element_type=F32)


def three_terms(v):
    hi = v.astype(BF16).astype(F32)
    mid = (v - hi).astype(BF16).astype(F32)
    low = (v - hi - mid).astype(BF16).astype(F32)
    return hi, mid, low


def in_hbm(v):
    return pltpu.with_memory_space_constraint(v, pltpu.HBM)


def sigmoid(v):
    return 1.0 / (1.0 + jnp.exp(-v))


def mixer_kernel(
    hidden_hbm, head_in_hbm, gate_hbm, b_hbm, c_hbm, raw_hbm, hist_hbm, taps_hbm,
    rate_hbm, extra_hbm, skip_hbm, index_hbm, weight_hbm, scale_hbm, state_hbm, wout_hbm,
    packed_ref, resid_ref, state_out, new_hist_out,
    hidden_ref, head_in_ref, gate_ref, b_ref, c_ref, raw_ref, hist_ref, taps_ref,
    rate_ref, extra_ref, skip_ref, index_ref, weight_ref, scale_ref, state_v, wout_v,
    lt, bt, dec_b, small_sem, in_sem, w_sem, out_sem, hist_sem,
):
    seqs, inner = head_in_ref.shape
    heads = raw_ref.shape[1]
    width = inner // heads
    groups = b_ref.shape[1] // STATE_DIM
    span = inner // groups
    full = hidden_ref.shape[1]
    topk = index_ref.shape[1]
    deep = lt.shape[1]

    small = [
        pltpu.make_async_copy(a, b, small_sem.at[i])
        for i, (a, b) in enumerate((
            (head_in_hbm, head_in_ref), (hist_hbm, hist_ref), (taps_hbm, taps_ref),
            (raw_hbm, raw_ref), (rate_hbm, rate_ref), (extra_hbm, extra_ref),
            (skip_hbm, skip_ref), (b_hbm, b_ref), (c_hbm, c_ref),
            (gate_hbm, gate_ref), (hidden_hbm, hidden_ref), (index_hbm, index_ref),
            (weight_hbm, weight_ref), (scale_hbm, scale_ref),
        ))
    ]
    for copy in small:
        copy.start()

    def group_rows(g):
        return pl.ds(g * span, span)

    def in_copy(g):
        return pltpu.make_async_copy(
            state_hbm.at[:, group_rows(g)], state_v.at[:, group_rows(g)], in_sem.at[g]
        )

    def out_copy(g, pair):
        where = (pl.ds(2 * pair, 2), group_rows(g))
        return pltpu.make_async_copy(state_v.at[where], state_out.at[where], out_sem.at[g, pair])

    def w_copy(g):
        return pltpu.make_async_copy(wout_hbm.at[group_rows(g)], wout_v.at[group_rows(g)], w_sem.at[g])

    in_copy(0).start()
    w_copy(0).start()
    in_copy(1).start()
    w_copy(1).start()

    for copy in small:
        copy.wait()
    hist_copies = (
        pltpu.make_async_copy(hist_ref.at[pl.ds(1, 2)], new_hist_out.at[pl.ds(0, 2)], hist_sem.at[0]),
        pltpu.make_async_copy(head_in_ref, new_hist_out.at[2], hist_sem.at[1]),
    )
    for copy in hist_copies:
        copy.start()
    taps = taps_ref[...].astype(F32)
    head_in = head_in_ref[...]
    total = head_in.astype(F32) * taps[3:4]
    for t in range(3):
        total = total + hist_ref[t].astype(F32) * taps[t:t + 1]
    conv = total * sigmoid(total)

    raw = raw_ref[...].astype(F32)
    step = jnp.maximum(raw, 0.0) + jnp.log(1.0 + jnp.exp(-jnp.abs(raw)))
    decay = jnp.exp(extra_ref[...] - rate_ref[...] * step)
    for h in range(heads):
        dec_b[h] = jnp.broadcast_to(decay[:, h:h + 1], (seqs, STATE_DIM))
    skip = jnp.broadcast_to(skip_ref[...], (seqs, heads))
    terms = jnp.concatenate(three_terms(step) + three_terms(skip) + three_terms(decay), axis=0).astype(BF16)
    spread = (
        lax.broadcasted_iota(jnp.int32, (heads, inner), 1) // width
        == lax.broadcasted_iota(jnp.int32, (heads, inner), 0)
    ).astype(F32).astype(BF16)
    wide = dot(terms, spread)

    def widened(i):
        at = 3 * i * seqs
        return wide[at:at + seqs] + wide[at + seqs:at + 2 * seqs] + wide[at + 2 * seqs:at + 3 * seqs]

    step_wide, skip_wide, decay_wide = widened(0), widened(1), widened(2)
    fed = step_wide * conv
    pad = jnp.zeros((deep - 3 * seqs, inner), F32)
    lt[...] = jnp.concatenate(three_terms(fed) + (pad,), axis=0).T.astype(BF16)
    b_all = b_ref[...].astype(F32)
    c_all = c_ref[...].astype(F32)
    b_rows = lax.broadcasted_iota(jnp.int32, (deep, LANES), 0)
    c_rows = lax.broadcasted_iota(jnp.int32, (seqs, STATE_DIM), 0)
    side = jnp.zeros((deep, LANES - STATE_DIM), F32)
    gate = gate_ref[...].astype(F32)
    gate = gate * sigmoid(gate)
    direct = []
    for g in range(groups):
        lanes = slice(g * STATE_DIM, (g + 1) * STATE_DIM)
        columns = slice(g * span, (g + 1) * span)
        b_g = b_all[:, lanes]
        tall = jnp.concatenate([b_g, b_g, b_g, jnp.zeros((deep - 3 * seqs, STATE_DIM), F32)], axis=0)
        tall = jnp.concatenate([tall, side], axis=1)
        for s in range(seqs):
            bt[g, :, s * LANES:(s + 1) * LANES] = jnp.where(b_rows % seqs == s, tall, 0.0).astype(BF16)
        met = jnp.sum(b_g * c_all[:, lanes], axis=1, keepdims=True)
        direct.append(fed[:, columns] * met + skip_wide[:, columns] * conv[:, columns])

    mixed = jnp.zeros((seqs, full), F32)
    for g in range(groups):
        columns = slice(g * span, (g + 1) * span)
        c_g = c_all[:, g * STATE_DIM:(g + 1) * STATE_DIM]
        in_copy(g).wait()
        if g + 2 < groups:
            in_copy(g + 2).start()
            w_copy(g + 2).start()
        read = jnp.zeros((seqs, span), F32)
        for pair in range(seqs // 2):
            outer = dot(lt[columns, :], bt[g, :, 2 * pair * LANES:2 * (pair + 1) * LANES])
            for k in range(2):
                s = 2 * pair + k
                old = state_v[s, columns, :].astype(BF16)
                picked = jnp.where(c_rows == s, c_g, 0.0).astype(BF16)
                read = read + lax.dot_general(picked, old, NT, preferred_element_type=F32)
                for j in range(span // width):
                    h = g * (span // width) + j
                    rows = slice(h * width, (h + 1) * width)
                    state_v[s, rows, :] = (
                        state_v[s, rows, :] * dec_b[h, s:s + 1, :]
                        + outer[j * width:(j + 1) * width, k * LANES:k * LANES + STATE_DIM]
                    )
            out_copy(g, pair).start()
        gated = ((decay_wide[:, columns] * read + direct[g]) * gate[:, columns]).astype(BF16)
        w_copy(g).wait()
        mixed = mixed + dot(gated, wout_v[columns, :])

    resid = (hidden_ref[...].astype(F32) + mixed.astype(BF16).astype(F32)).astype(BF16)
    resid_ref[...] = resid
    values = resid.astype(F32)
    inv_rms = lax.rsqrt(jnp.mean(values * values, axis=1, keepdims=True) + EPSILON)
    scale = scale_ref[...].reshape(1, full).astype(F32)
    packed_ref[:, :full] = (values * scale).astype(BF16)

    lane = lax.broadcasted_iota(jnp.int32, (seqs, LANES), 1)
    dense = jnp.zeros((seqs, LANES), F32)
    index, weight = index_ref[...], weight_ref[...]
    for k in range(topk):
        dense = dense + jnp.where(lane % FIELD == index[:, k:k + 1], weight[:, k:k + 1], 0.0)
    high = dense.astype(BF16).astype(F32)
    extras = jnp.where(lane < FIELD, high, dense - high)
    for t, term in enumerate(three_terms(inv_rms)):
        extras = jnp.where(lane == 2 * FIELD + t, term, extras)
    packed_ref[:, full:] = extras.astype(BF16)
    for g in range(groups):
        for pair in range(seqs // 2):
            out_copy(g, pair).wait()
    for copy in hist_copies:
        copy.wait()


def expert_kernel(
    n_ep, packed_ref, resid_ref, wg_hbm, wu_hbm, wd_hbm, out_ref,
    wg, wu, wd, rows_in, act, sent, pair_in, over, over_in, along, along_in,
    w_sem, own_sem, cross_sem, relay_sem, recv_sem, pair_send, pair_recv,
    over_send, over_recv, along_send, along_recv,
):
    me = lax.axis_index("ep")
    line = n_ep // 4
    at, side, core = me // 4, me // 2 % 2, me % 2
    seqs, full = out_ref.shape

    def device(z, x, c):
        return z * 4 + x * 2 + c

    def other(d):
        return (at + d) % line

    partner = device(at, side, 1 - core)
    across = device(at, 1 - side, core)
    barrier = pltpu.get_barrier_semaphore()
    peers = [partner, across] + [device(other(d), side, core) for d in range(1, line)]
    for peer in peers:
        pl.semaphore_signal(barrier, inc=1, device_id={"ep": peer}, device_id_type=MESH)
    weights = [
        pltpu.make_async_copy(a, b, w_sem.at[i])
        for i, (a, b) in enumerate(((wg_hbm, wg), (wu_hbm, wu), (wd_hbm, wd)))
    ]
    for copy in weights:
        copy.start()
    pl.semaphore_wait(barrier, len(peers))

    def remote(src, dst, send, recv, target):
        return pltpu.make_async_remote_copy(
            src_ref=src, dst_ref=dst, send_sem=send, recv_sem=recv,
            device_id={"ep": target}, device_id_type=MESH,
        )

    def slot(z, x, c):
        return (c * 2 + x) * line + z

    def arrived(where):
        remote(packed_ref, rows_in.at[where], own_sem.at[0], recv_sem.at[where], partner).wait_recv()

    started = []

    def start(copy):
        copy.start()
        started.append(copy)

    def forward(where, sem, target):
        start(remote(rows_in.at[where], rows_in.at[where], sem, recv_sem.at[where], target))

    mine = slot(at, side, core)
    for d in range(1, line):
        start(remote(packed_ref, rows_in.at[mine], own_sem.at[d], recv_sem.at[mine], peers[1 + d]))
    start(remote(packed_ref, rows_in.at[mine], own_sem.at[0], recv_sem.at[mine], across))
    start(remote(packed_ref, rows_in.at[mine], own_sem.at[line], recv_sem.at[mine], partner))
    rows_in[mine] = packed_ref[...]

    arrived(slot(at, 1 - side, core))
    forward(slot(at, 1 - side, core), relay_sem.at[0], partner)
    for d in range(line - 1, 0, -1):
        where = slot(other(d), side, core)
        arrived(where)
        forward(where, cross_sem.at[d], across)
        forward(where, relay_sem.at[d], partner)
    for d in range(line - 1, 0, -1):
        where = slot(other(d), 1 - side, core)
        arrived(where)
        forward(where, relay_sem.at[line - 1 + d], partner)
    for x in (side, 1 - side):
        for d in range(line):
            arrived(slot(other(d), x, 1 - core))

    values = rows_in[...].astype(F32).reshape(n_ep * seqs, full + LANES)
    scaled = values[:, :full].astype(BF16)
    extras = values[:, full:]
    lane = lax.broadcasted_iota(jnp.int32, (n_ep * seqs, LANES), 1)

    def total_of(mask):
        return jnp.sum(jnp.where(mask, extras, 0.0), axis=1, keepdims=True)

    share = total_of((lane < 2 * FIELD) & (lane % FIELD == me))
    inv_rms = total_of((lane >= 2 * FIELD) & (lane < 2 * FIELD + 3))
    weights[0].wait()
    pre_gate = inv_rms * lax.dot_general(scaled, wg[...], NT, preferred_element_type=F32)
    weights[1].wait()
    pre_up = inv_rms * lax.dot_general(scaled, wu[...], NT, preferred_element_type=F32)
    act[...] = (pre_gate * sigmoid(pre_gate) * pre_up).astype(BF16)
    weights[2].wait()
    down = dot(act[...], wd[...]).astype(BF16).astype(F32) * share
    sent[...] = down.astype(BF16).reshape(2, 2, line, seqs, full)

    pairs = [
        remote(sent.at[1 - core, x], pair_in.at[x], pair_send.at[i], pair_recv.at[i], partner)
        for i, x in enumerate((1 - side, side))
    ]
    for copy in pairs:
        start(copy)
    pairs[0].wait_recv()
    overs = []
    for d in range(1, line + 1):
        z = other(d)
        over[z] = (sent[core, 1 - side, z].astype(F32) + pair_in[1 - side, z].astype(F32)).astype(BF16)
        overs.append(remote(over.at[z], over_in.at[z], over_send.at[d - 1], over_recv.at[d - 1], across))
        start(overs[-1])
    pairs[1].wait_recv()
    for d in range(1, line):
        z = other(d)
        overs[d - 1].wait_recv()
        here = sent[core, side, z].astype(F32) + pair_in[side, z].astype(F32)
        along[d] = (here + over_in[z].astype(F32)).astype(BF16)
        start(
            remote(along.at[d], along_in.at[d], along_send.at[d], along_recv.at[d], peers[1 + d])
        )
    total = resid_ref[...].astype(F32)
    total = total + sent[core, side, at].astype(F32) + pair_in[side, at].astype(F32)
    overs[line - 1].wait_recv()
    total = total + over_in[at].astype(F32)
    for d in range(1, line):
        remote(along.at[d], along_in.at[d], along_send.at[d], along_recv.at[d], peers[1]).wait_recv()
        total = total + along_in[d].astype(F32)
    out_ref[...] = total.astype(BF16)
    for copy in started:
        copy.wait_send()


def on_device_kernels(
    n_ep,
    hidden,
    head_input_projected,
    output_gate_projected,
    input_map_projected,
    output_map_projected,
    raw_step_size,
    convolution_history,
    convolution_kernel,
    recurrent_state_matrix,
    head_decay_rate,
    extra_log_decay,
    head_skip_weight,
    output_matrix,
    expert_norm_scale,
    token_expert_index,
    token_expert_weight,
    expert_gate_weight,
    expert_up_weight,
    expert_down_weight,
):
    seqs, full = hidden.shape
    inner = head_input_projected.shape[1]
    heads = raw_step_size.shape[1]
    groups = input_map_projected.shape[1] // STATE_DIM
    hidden_units = expert_down_weight.shape[1]
    line = n_ep // 4
    taps = convolution_history.shape[1]
    state = recurrent_state_matrix.reshape(seqs, inner, STATE_DIM)
    deep = 4 * seqs
    dma = pltpu.SemaphoreType.DMA
    operands = (
        hidden, head_input_projected, output_gate_projected, input_map_projected,
        output_map_projected, raw_step_size, jnp.swapaxes(convolution_history, 0, 1),
        convolution_kernel, head_decay_rate.reshape(1, heads), extra_log_decay,
        head_skip_weight.reshape(1, heads), token_expert_index, token_expert_weight,
        expert_norm_scale, state, output_matrix,
    )
    packed, resid, new_state, new_hist = pl.pallas_call(
        mixer_kernel,
        out_shape=(
            pltpu.VMEM((seqs, full + LANES), BF16),
            pltpu.VMEM((seqs, full), BF16),
            pltpu.HBM(state.shape, F32),
            pltpu.HBM((taps, seqs, inner), BF16),
        ),
        in_specs=[HBM_SPEC] * len(operands),
        out_specs=(VMEM_SPEC, VMEM_SPEC, HBM_SPEC, HBM_SPEC),
        scratch_shapes=[pltpu.VMEM(v.shape, v.dtype) for v in operands] + [
            pltpu.VMEM((inner, deep), BF16),
            pltpu.VMEM((groups, deep, seqs * LANES), BF16),
            pltpu.VMEM((heads, seqs, STATE_DIM), F32),
            dma((len(operands) - 2,)),
            dma((groups,)),
            dma((groups,)),
            dma((groups, seqs // 2)),
            dma((2,)),
        ],
        compiler_params=pltpu.CompilerParams(vmem_limit_bytes=MIXER_VMEM),
        name="mixer",
    )(*[in_hbm(v) for v in operands])
    block = (seqs, full)
    layer_out = pl.pallas_call(
        functools.partial(expert_kernel, n_ep),
        out_shape=jax.ShapeDtypeStruct(block, BF16),
        in_specs=[VMEM_SPEC] * 2 + [HBM_SPEC] * 3,
        out_specs=VMEM_SPEC,
        scratch_shapes=[pltpu.VMEM((hidden_units, full), BF16)] * 3 + [
            pltpu.VMEM((n_ep, seqs, full + LANES), BF16),
            pltpu.VMEM((n_ep * seqs, hidden_units), BF16),
            pltpu.VMEM((2, 2, line) + block, BF16),
            pltpu.VMEM((2, line) + block, BF16),
            pltpu.VMEM((line,) + block, BF16),
            pltpu.VMEM((line,) + block, BF16),
            pltpu.VMEM((line,) + block, BF16),
            pltpu.VMEM((line,) + block, BF16),
            dma((3,)),
            dma((line + 1,)),
            dma((line,)),
            dma((2 * line - 1,)),
            dma((n_ep,)),
            dma((2,)),
            dma((2,)),
            dma((line,)),
            dma((line,)),
            dma((line,)),
            dma((line,)),
        ],
        compiler_params=pltpu.CompilerParams(
            collective_id=0, has_side_effects=True, vmem_limit_bytes=EXPERT_VMEM
        ),
        name="experts",
    )(
        packed, resid, in_hbm(jnp.swapaxes(expert_gate_weight[0], 0, 1)),
        in_hbm(jnp.swapaxes(expert_up_weight[0], 0, 1)), in_hbm(expert_down_weight[0]),
    )
    return (
        layer_out, new_state.reshape(recurrent_state_matrix.shape), jnp.swapaxes(new_hist, 0, 1)
    )


def solution(mesh):
    n_ep = mesh.shape["ep"]
    whole_heads = mesh.shape["tp"] == 1 and n_ep % 4 == 0 and 4 < n_ep <= FIELD
    body = functools.partial(on_device_kernels, n_ep) if whole_heads else on_device
    in_specs = (
        P(("grp", "ep"), "tp"),
        P(("grp", "ep"), "tp"),
        P(("grp", "ep"), "tp"),
        P(("grp", "ep"), "tp"),
        P(("grp", "ep"), "tp"),
        P(("grp", "ep"), "tp"),
        P(("grp", "ep"), None, "tp"),
        P(None, "tp"),
        P(("grp", "ep"), "tp", None, None),
        P("tp"),
        P(("grp", "ep"), "tp"),
        P("tp"),
        P("tp", None),
        P(),
        P(("grp", "ep"), None),
        P(("grp", "ep"), None),
        P("ep", None, "tp"),
        P("ep", None, "tp"),
        P("ep", "tp", None),
    )
    out_specs = (
        P(("grp", "ep"), "tp"),
        P(("grp", "ep"), "tp", None, None),
        P(("grp", "ep"), None, "tp"),
    )
    return jax.shard_map(
        body, mesh=mesh, in_specs=in_specs, out_specs=out_specs, check_vma=False
    )
```
